32 devices in a mesh: ep: 16 (over z, y, x), tp: 2 (over core).
Axes of the slice: x: 2, y: 2, z: 4, core: 2. Of those that a mesh axis runs over, the one named last changes fastest.
Arguments:
- stream: bfloat16 [512, 2048], P('ep'), may hold values from -6 to 6
- mixer_gain: float32 [2048], replicated, may hold values from 0.1 to 1.9
- gate_proj: bfloat16 [2048, 1024], P(None, 'tp'), may hold values from -0.125 to 0.125
- input_proj: bfloat16 [2048, 1024], P(None, 'tp'), may hold values from -0.125 to 0.125
- state_maps: bfloat16 [2, 2048, 256], P(None, None, 'tp'), may hold values from -0.125 to 0.125
- step_proj: bfloat16 [2048, 16], P(None, 'tp'), may hold values from -0.125 to 0.125
- step_bias: float32 [16], P('tp'), may hold values from -3 to 0.5
- decay_rate: float32 [16], P('tp'), may hold values from 0.05 to 4
- input_taps: float32 [4, 1024], P(None, 'tp'), may hold values from -3 to 3
- map_taps: float32 [2, 4, 256], P(None, None, 'tp'), may hold values from -3 to 3
- input_past: bfloat16 [512, 3, 1024], P('ep', None, 'tp'), may hold values from -6 to 6
- map_past: bfloat16 [512, 2, 3, 256], P('ep', None, None, 'tp'), may hold values from -6 to 6
- head_state: float32 [512, 16, 4096], P('ep', 'tp'), may hold values from -1.6 to 1.6
- skip_gain: float32 [16], P('tp'), may hold values from 0 to 2
- inner_gain: float32 [1024], P('tp'), may hold values from 0.1 to 1.9
- mixer_out: bfloat16 [1024, 2048], P('tp'), may hold values from -0.1875 to 0.1875
- channel_gain: float32 [2048], replicated, may hold values from 0.1 to 1.9
- expert_ids: int32 [512, 2], P('ep'), may hold values from 0 to 7, all different within a row; in each aligned block of 32 rows (0 to 31, 32 to 63, ...) at most 12 rows name the same one
- expert_weight: float32 [512, 2], P('ep'), may hold values from 0.2 to 1
- expert_gate: bfloat16 [2048, 57344], P(None, ('ep', 'tp')), may hold values from -0.125 to 0.125
- expert_up: bfloat16 [2048, 57344], P(None, ('ep', 'tp')), may hold values from -0.125 to 0.125
- expert_down: bfloat16 [57344, 2048], P(('ep', 'tp')), may hold values from -0.0625 to 0.0625
- dense_gate: bfloat16 [2048, 5632], P('tp', 'ep'), may hold values from -0.125 to 0.125
- dense_up: bfloat16 [2048, 5632], P('tp', 'ep'), may hold values from -0.125 to 0.125
- dense_down: bfloat16 [5632, 2048], P('ep', 'tp'), may hold values from -0.078125 to 0.078125
- dense_mix: float32 [2048], P('tp'), may hold values from -2 to 2
Outputs:
- stream_out: bfloat16 [512, 2048], P('ep', 'tp')
- state_out: float32 [512, 16, 4096], P('ep', 'tp')
The draws below stay inside these ranges and needn't reach their ends.
Inputs may be any that keep to these rules, and one draw needn't show every extreme that they name: `expert_ids`: each row names 2 different experts. In each aligned block of 32 rows no expert is named by more than 12 rows, and in some block one expert is named by exactly 12 rows.
All inputs are finite; a program needn't handle non-finite values.
Results may differ from the reference program's by a relative error of at most 0.015.
Values may be sent and summed in bfloat16 or wider, within the bound.
No kernel may reach another device: no remote copies, remote signals or barrier semaphores. Data moves between devices by JAX's collectives and lax.ppermute only.
A program may use at most 128 MiB of HBM per device.

```python
import math
import jax
import jax.numpy as jnp
import numpy as np
from jax import lax

D = 2048
INNER = 1024
HEAD = 64
HEADS = 16
GROUPS = 4
NSTATE = 64
CONV = 4
EXPERTS = 8
TOP_K = 2
EXPERT_HIDDEN = 7168
DENSE_HIDDEN = 5632
SEQ_DEV = 32
BATCH = 512
CAP = 12
N_EP = 16
N_TP = 2


def steps_of(stream_key, dims, shards, low, high):
    level = 1.0
    for dim, blocks in shards:
        heights = jax.random.uniform(jax.random.fold_in(jax.random.fold_in(stream_key, 6), dim), (blocks,), jnp.float32, low / len(shards), high / len(shards))
        level = level * jnp.repeat(jnp.exp(heights), dims[dim] // blocks).reshape((-1,) + (1,) * (len(dims) - 1 - dim))
    return level


def shared_out(stream_key, own, number, rows, amount, top, limit, skew):
    ranking = jax.random.permutation(stream_key, amount)
    packed, common = portions_of(amount, rows * top, limit, skew, True), portions_of(amount, rows * top, limit, skew, False)
    places = jnp.arange(amount)

    def named(sizes, turn):
        used = int((sizes > 0).sum())
        fixed = max(1, used // 4)
        passed = fixed + (places - fixed + turn * (used - fixed)) % max(1, amount - fixed)
        return jnp.zeros((amount,), jnp.int32).at[ranking[jnp.where(places < fixed, places, passed)]].set(jnp.asarray(sizes, jnp.int32))

    sizes = jnp.where(number % 4 == 0, named(packed, number // 4), named(common, number - number // 4 - 1))
    mixed = jax.random.permutation(jax.random.fold_in(own, 3), amount)
    source_of, taker = mixed[0:amount // 2 * 2:2], mixed[1:amount // 2 * 2:2]
    slack = jnp.minimum(sizes[source_of] - 1, limit - sizes[taker]) // 2
    slack = jnp.where((source_of == ranking[0]) | (taker == ranking[0]) | (sizes[taker] == 0), 0, jnp.maximum(slack, 0))
    passed = jax.random.randint(jax.random.fold_in(own, 4), (amount // 2,), 0, 1 << 20) % (slack + 1)
    sizes = sizes.at[source_of].add(-passed).at[taker].add(passed)
    items = jnp.searchsorted(jnp.cumsum(sizes), jnp.arange(rows * top), side="right").astype(jnp.int32)
    table = items.reshape(top, rows).T
    table = table[jax.random.permutation(jax.random.fold_in(own, 1), rows)]
    turn = jax.random.randint(jax.random.fold_in(own, 2), (rows, 1), 0, top)
    return jnp.take_along_axis(table, (jnp.arange(top)[None, :] + turn) % top, axis=1)


def portions_of(amount, total, most, skew, full):
    weights = [(1 << 20) // math.isqrt(rank ** skew) + 1 for rank in range(1, amount + 1)]
    largest = most if full else min(most, max(-(-total // amount), total * weights[0] // sum(weights)))
    least = 1 if total - largest >= amount - 1 else 0
    counts, rest = [largest] + [least] * (amount - 1), total - largest - least * (amount - 1)
    while rest > 0:
        free = [i for i in range(1, amount) if counts[i] < largest] or [i for i in range(1, amount) if counts[i] < most]
        whole, left = sum([weights[i] for i in free]), rest
        for i in free:
            extra = min(most - counts[i], max(1, left * weights[i] // whole), rest)
            counts[i] = counts[i] + extra
            rest = rest - extra
    return np.array(counts)


def noise(rng, shape, width, reach, pieces=(), kind=jnp.bfloat16):
    values = width * jax.random.normal(rng, shape, jnp.float32)
    if pieces:
        values = values * steps_of(rng, shape, pieces, -0.22, 0.18)
    return jnp.clip(values, -reach, reach).astype(kind)


def setup_inputs(seed: int = 0) -> dict:
    key_list = jax.random.split(jax.random.key(seed), 27)
    stream = noise(key_list[0], (BATCH, D), 1.0, 6.0, ((0, 16),))
    mixer_gain = jnp.clip(1.0 + 0.18 * jax.random.normal(key_list[1], (D,), jnp.float32), 0.1, 1.9)
    gate_proj = noise(key_list[2], (D, INNER), D ** -0.5, 0.125, ((1, 2),))
    input_proj = noise(key_list[3], (D, INNER), D ** -0.5, 0.125, ((1, 2),))
    state_maps = noise(key_list[4], (2, D, GROUPS * NSTATE), D ** -0.5, 0.125, ((2, 2),))
    step_proj = noise(key_list[5], (D, HEADS), D ** -0.5, 0.125, ((1, 2),))
    step_bias = jnp.clip(-3.0 + 3.5 * jax.random.uniform(key_list[6], (HEADS,), jnp.float32) ** steps_of(key_list[6], (HEADS,), ((0, 2),), -0.2, 0.2), -3.0, 0.5)
    decay_rate = jnp.clip(jnp.exp(math.log(4.0) - 4.3820266 * jax.random.uniform(key_list[7], (HEADS,), jnp.float32) ** steps_of(key_list[7], (HEADS,), ((0, 2),), -0.2, 0.2)), 0.05, 4.0)
    input_taps = noise(key_list[8], (CONV, INNER), 0.5, 3.0, ((1, 2),), jnp.float32)
    map_taps = noise(key_list[9], (2, CONV, GROUPS * NSTATE), 0.5, 3.0, ((2, 2),), jnp.float32)
    input_past = noise(key_list[10], (BATCH, CONV - 1, INNER), 1.0, 6.0, ((0, 16), (2, 2)))
    map_past = noise(key_list[11], (BATCH, 2, CONV - 1, GROUPS * NSTATE), 1.0, 6.0, ((0, 16), (3, 2)))
    head_state = noise(key_list[12], (BATCH, HEADS, HEAD * NSTATE), 0.2, 1.6, ((0, 16), (1, 2)), jnp.float32)
    skip_gain = jnp.clip(2.0 * jax.random.uniform(key_list[13], (HEADS,), jnp.float32) ** steps_of(key_list[13], (HEADS,), ((0, 2),), -0.2, 0.2), 0.0, 2.0)
    inner_gain = jnp.clip(1.0 + 0.18 * jax.random.normal(key_list[14], (INNER,), jnp.float32), 0.1, 1.9)
    mixer_out = noise(key_list[15], (INNER, D), INNER ** -0.5, 0.1875, ((0, 2),))
    channel_gain = jnp.clip(1.0 + 0.18 * jax.random.normal(key_list[16], (D,), jnp.float32), 0.1, 1.9)
    expert_ids_keys = jax.random.split(jax.random.fold_in(key_list[17], 1), BATCH // SEQ_DEV)
    expert_ids_turns = jax.random.permutation(jax.random.fold_in(key_list[17], 3), BATCH // SEQ_DEV)
    expert_ids = jax.vmap(lambda own, number: shared_out(jax.random.fold_in(key_list[17], 2), own, number, SEQ_DEV, EXPERTS, TOP_K, CAP, 2))(expert_ids_keys, expert_ids_turns).reshape((BATCH, TOP_K))
    expert_weight = jnp.clip(0.2 + 0.8 * jax.random.uniform(key_list[18], (BATCH, TOP_K), jnp.float32) ** steps_of(key_list[18], (BATCH, TOP_K), ((0, 16),), -0.2, 0.2), 0.2, 1.0)
    expert_gate = noise(key_list[19], (D, EXPERTS * EXPERT_HIDDEN), D ** -0.5, 0.125, ((1, 32),))
    expert_up = noise(key_list[20], (D, EXPERTS * EXPERT_HIDDEN), D ** -0.5, 0.125, ((1, 32),))
    expert_down = noise(key_list[21], (EXPERTS * EXPERT_HIDDEN, D), EXPERT_HIDDEN ** -0.5, 0.0625, ((0, 32),))
    dense_gate = noise(key_list[22], (D, DENSE_HIDDEN), D ** -0.5, 0.125, ((0, 2), (1, 16)))
    dense_up = noise(key_list[23], (D, DENSE_HIDDEN), D ** -0.5, 0.125, ((0, 2), (1, 16)))
    dense_down = noise(key_list[24], (DENSE_HIDDEN, D), DENSE_HIDDEN ** -0.5, 0.078125, ((0, 16), (1, 2)))
    dense_mix = jnp.clip(jax.random.uniform(key_list[25], (D,), jnp.float32, -2.0, 2.0) * steps_of(key_list[25], (D,), ((0, 2),), -0.4, 0.0), -2.0, 2.0)
    return {"stream": stream, "mixer_gain": mixer_gain, "gate_proj": gate_proj, "input_proj": input_proj, "state_maps": state_maps, "step_proj": step_proj, "step_bias": step_bias, "decay_rate": decay_rate, "input_taps": input_taps, "map_taps": map_taps, "input_past": input_past, "map_past": map_past, "head_state": head_state, "skip_gain": skip_gain, "inner_gain": inner_gain, "mixer_out": mixer_out, "channel_gain": channel_gain, "expert_ids": expert_ids, "expert_weight": expert_weight, "expert_gate": expert_gate, "expert_up": expert_up, "expert_down": expert_down, "dense_gate": dense_gate, "dense_up": dense_up, "dense_down": dense_down, "dense_mix": dense_mix}


EPS = 1e-06

def rms_scale(values):
    return values * lax.rsqrt(lax.optimization_barrier(jnp.mean(values * values, axis=-1, keepdims=True)) + EPS)

def short_conv(past_rows, newest, tap_weights, along):
    window = jnp.concatenate([past_rows, jnp.expand_dims(newest, along)], axis=along).astype(jnp.float32)
    return jax.nn.silu(lax.optimization_barrier(jnp.sum(window * tap_weights, axis=along)))

def mix_heads(stream, mixer_gain, gate_proj, input_proj, state_maps, step_proj, step_bias, decay_rate, input_taps, map_taps, input_past, map_past, head_state, skip_gain, inner_gain):
    row_count = stream.shape[0]
    normed = (rms_scale(stream.astype(jnp.float32)) * mixer_gain).astype(jnp.bfloat16)
    gate_in = jnp.dot(normed, gate_proj, preferred_element_type=jnp.float32).astype(jnp.bfloat16)
    input_new = jnp.dot(normed, input_proj, preferred_element_type=jnp.float32).astype(jnp.bfloat16)
    map_new = jnp.stack([jnp.dot(normed, state_maps[0], preferred_element_type=jnp.float32), jnp.dot(normed, state_maps[1], preferred_element_type=jnp.float32)], axis=1).astype(jnp.bfloat16)
    step_size = jax.nn.softplus(jnp.dot(normed, step_proj, preferred_element_type=jnp.float32) + step_bias)
    conv_in = short_conv(input_past, input_new, input_taps, 1)
    conv_map = short_conv(map_past, map_new, map_taps, 2)
    head_count = step_size.shape[1]
    per_group = HEADS // GROUPS
    group_count = head_count // per_group
    write_map = jnp.repeat(conv_map[:, 0].reshape(row_count, group_count, NSTATE), per_group, axis=1)
    read_map = jnp.repeat(conv_map[:, 1].reshape(row_count, group_count, NSTATE), per_group, axis=1)
    values = conv_in.reshape(row_count, head_count, HEAD)
    decay_now = jnp.exp(-decay_rate * step_size)
    state_old = head_state.reshape(row_count, head_count, HEAD, NSTATE)
    state_new = decay_now[:, :, None, None] * state_old + (step_size[:, :, None] * values)[:, :, :, None] * write_map[:, :, None, :]
    gated = lax.optimization_barrier(jnp.sum(state_new * read_map[:, :, None, :], axis=3)) + skip_gain[:, None] * values
    gated = gated.reshape(row_count, head_count * HEAD) * jax.nn.silu(gate_in.astype(jnp.float32))
    inner_out = rms_scale(gated.reshape(row_count, group_count, -1)).reshape(row_count, -1) * inner_gain
    return (inner_out.astype(jnp.bfloat16), state_new.reshape(row_count, head_count, HEAD * NSTATE))

def expert_sum(ffn_in, expert_ids, expert_weight, expert_gate, expert_up, expert_down):
    total_rows, feature_count = ffn_in.shape
    hidden = expert_gate.shape[1] // EXPERTS
    row_limit = min(total_rows, N_EP * CAP)

    def visit(running, expert_index):
        matched = expert_ids == expert_index
        chosen = jnp.any(matched, axis=1)
        weight = lax.optimization_barrier(jnp.sum(jnp.where(matched, expert_weight, jnp.zeros_like(expert_weight)), axis=1))
        picked = jnp.nonzero(chosen, size=row_limit, fill_value=0)[0].astype(jnp.int32)
        is_live = jnp.arange(row_limit, dtype=jnp.int32) < jnp.sum(chosen.astype(jnp.int32))
        taken_rows = ffn_in[picked]
        first_col = (expert_index * hidden).astype(jnp.int32)
        w_gate = lax.dynamic_slice_in_dim(expert_gate, first_col, hidden, 1)
        w_up = lax.dynamic_slice_in_dim(expert_up, first_col, hidden, 1)
        w_down = lax.dynamic_slice_in_dim(expert_down, first_col, hidden, 0)
        act = (jax.nn.silu(jnp.dot(taken_rows, w_gate, preferred_element_type=jnp.float32)) * jnp.dot(taken_rows, w_up, preferred_element_type=jnp.float32)).astype(jnp.bfloat16)
        result = jnp.dot(act, w_down, preferred_element_type=jnp.float32)
        scale = jnp.where(is_live, weight[picked], jnp.zeros_like(weight[picked]))
        return (running.at[picked].add(result * scale[:, None]), None)
    start_sum = jnp.zeros((total_rows, feature_count), jnp.float32)
    total, _ = lax.scan(visit, start_sum, jnp.arange(EXPERTS, dtype=jnp.int32))
    return total

def reference(stream, mixer_gain, gate_proj, input_proj, state_maps, step_proj, step_bias, decay_rate, input_taps, map_taps, input_past, map_past, head_state, skip_gain, inner_gain, mixer_out, channel_gain, expert_ids, expert_weight, expert_gate, expert_up, expert_down, dense_gate, dense_up, dense_down, dense_mix):
    inner_out, state_out = mix_heads(stream, mixer_gain, gate_proj, input_proj, state_maps, step_proj, step_bias, decay_rate, input_taps, map_taps, input_past, map_past, head_state, skip_gain, inner_gain)
    block_cols = inner_out.shape[1] // N_TP
    mixed = jnp.zeros((stream.shape[0], mixer_out.shape[1]), jnp.float32)
    for portion in range(N_TP):
        partial_out = jnp.dot(inner_out[:, portion * block_cols:(portion + 1) * block_cols], mixer_out[portion * block_cols:(portion + 1) * block_cols], preferred_element_type=jnp.float32)
        mixed = mixed + lax.optimization_barrier(partial_out.astype(jnp.bfloat16)).astype(jnp.float32)
    hidden_mid = stream.astype(jnp.float32) + mixed
    ffn_in = (rms_scale(hidden_mid) * channel_gain).astype(jnp.bfloat16)
    routed = expert_sum(ffn_in, expert_ids, expert_weight, expert_gate, expert_up, expert_down)
    dense_act = (jax.nn.silu(jnp.dot(ffn_in, dense_gate, preferred_element_type=jnp.float32)) * jnp.dot(ffn_in, dense_up, preferred_element_type=jnp.float32)).astype(jnp.bfloat16)
    dense_res = jnp.dot(dense_act, dense_down, preferred_element_type=jnp.float32)
    stream_out = (hidden_mid + routed + jax.nn.sigmoid(dense_mix) * dense_res).astype(jnp.bfloat16)
    return (stream_out, state_out)
```

```python
import math
import jax
import jax.numpy as jnp
from jax import lax
from jax.experimental import pallas as pl
from jax.experimental.pallas import tpu as pltpu
from jax.sharding import PartitionSpec as P

HEAD = 64
HEADS = 16
GROUPS = 4
NSTATE = 64
EXPERTS = 8
TOP_K = 2
CAP = 12


EPS = 1e-06


def rms_scale(values):
    return values * lax.rsqrt(jnp.mean(values * values, axis=-1, keepdims=True) + EPS)


def ring_dims(count):
    side = math.isqrt(count // 4)
    if 4 * side * side == count and side in (2, 4):
        return (4, side, side)
    dims = []
    while count > 1:
        assert count % 2 == 0
        dims.append(2)
        count //= 2
    return tuple(dims)


def shift(values, dims, k, offset):
    stride = math.prod(dims[k + 1 :])
    size = dims[k]
    pairs = []
    for d in range(math.prod(dims)):
        c = d // stride % size
        pairs.append((d, d + ((c + offset) % size - c) * stride))
    return lax.ppermute(values, "ep", pairs)


def gather_rows(x, dims):
    for k in reversed(range(len(dims))):
        if dims[k] == 2:
            x = jnp.concatenate([x, shift(x, dims, k, 1)], axis=0)
        else:
            half = x.shape[0] // 2
            a = shift(x, dims, k, 1)
            b = shift(x, dims, k, -1)
            c = shift(a[:half], dims, k, 1)
            d = shift(b[half:], dims, k, -1)
            x = jnp.concatenate([x, a, b, c, d], axis=0)
    return x


def scatter_rows(y, dims):
    def sent(v, k, offset):
        return shift(v.astype(jnp.bfloat16), dims, k, offset).astype(jnp.float32)

    for k in range(len(dims)):
        m = y.shape[0] // dims[k]
        if dims[k] == 2:
            y = y[:m] + sent(y[m:], k, 1)
        else:
            half = m // 2
            rc = sent(y[3 * m : 3 * m + half], k, -1)
            rd = sent(y[3 * m + half :], k, 1)
            a = y[m : 2 * m]
            b = y[2 * m : 3 * m]
            a = jnp.concatenate([a[:half] + rc, a[half:]], axis=0)
            b = jnp.concatenate([b[:half], b[half:] + rd], axis=0)
            y = y[:m] + sent(a, k, -1) + sent(b, k, 1)
    return y


def swap_cores(values):
    return lax.ppermute(values, "tp", [(0, 1), (1, 0)])


def split_dot(values, table, dims):
    high = values.astype(jnp.bfloat16)
    low = (values - high.astype(jnp.float32)).astype(jnp.bfloat16)
    return lax.dot_general(
        high, table, (dims, ((), ())), preferred_element_type=jnp.float32
    ) + lax.dot_general(low, table, (dims, ((), ())), preferred_element_type=jnp.float32)


def tiled_lanes(row, width):
    return jnp.concatenate([row] * (width // row.shape[1]), axis=1)


def read_body(state_ref, read_ref, spread_ref, out_ref):
    product = state_ref[...] * tiled_lanes(read_ref[...], state_ref.shape[1])
    out_ref[...] = split_dot(product, spread_ref[...], ((1,), (1,)))


def write_body(state_ref, decay_ref, value_ref, write_ref, spread_ref, out_ref):
    value = split_dot(value_ref[...], spread_ref[...], ((1,), (0,)))
    write = tiled_lanes(write_ref[...], state_ref.shape[1])
    out_ref[...] = decay_ref[...] * state_ref[...] + value * write


def rows_spec(block, width):
    return pl.BlockSpec((block, width), lambda i: (i, 0))


def read_state(state, read2, spread):
    rows, width = state.shape
    block = 64
    return pl.pallas_call(
        read_body,
        grid=(rows // block,),
        in_specs=[
            rows_spec(block, width),
            rows_spec(block, read2.shape[1]),
            pl.BlockSpec(spread.shape, lambda i: (0, 0)),
        ],
        out_specs=rows_spec(block, HEAD),
        out_shape=jax.ShapeDtypeStruct((rows, HEAD), jnp.float32),
        name="read_state",
    )(state, read2, spread)


def write_state(state, decay, value, write2, spread):
    rows, width = state.shape
    block = 64
    return pl.pallas_call(
        write_body,
        grid=(rows // block,),
        in_specs=[
            rows_spec(block, width),
            rows_spec(block, 1),
            rows_spec(block, HEAD),
            rows_spec(block, write2.shape[1]),
            pl.BlockSpec(spread.shape, lambda i: (0, 0)),
        ],
        out_specs=rows_spec(block, width),
        out_shape=jax.ShapeDtypeStruct((rows, width), jnp.float32),
        name="write_state",
    )(state, decay, value, write2, spread)


def project(rows, weight):
    return jnp.dot(rows, weight, preferred_element_type=jnp.float32)


def local(
    stream,
    mixer_gain,
    gate_proj,
    input_proj,
    state_maps,
    step_proj,
    step_bias,
    decay_rate,
    input_taps,
    map_taps,
    input_past,
    map_past,
    head_state,
    skip_gain,
    inner_gain,
    mixer_out,
    channel_gain,
    expert_ids,
    expert_weight,
    expert_gate,
    expert_up,
    expert_down,
    dense_gate,
    dense_up,
    dense_down,
    dense_mix,
):
    ep_size = lax.axis_size("ep")
    dims = ring_dims(ep_size)
    core = lax.axis_index("tp")
    gate_other = swap_cores(dense_gate)
    up_other = swap_cores(dense_up)
    row_count, feature_count = stream.shape
    named = gather_rows(
        jnp.concatenate([expert_ids.astype(jnp.float32), expert_weight], axis=1), dims
    )

    normed = (rms_scale(stream.astype(jnp.float32)) * mixer_gain).astype(jnp.bfloat16)
    maps = []
    for m in range(2):
        new = project(normed, state_maps[m]).astype(jnp.bfloat16).astype(jnp.float32)
        total = map_taps[m, 3] * new
        for t in range(3):
            total = total + map_taps[m, t] * map_past[:, m, t].astype(jnp.float32)
        maps.append(jax.nn.silu(total))
    input_new = project(normed, input_proj).astype(jnp.bfloat16).astype(jnp.float32)
    total = input_taps[3] * input_new
    for t in range(3):
        total = total + input_taps[t] * input_past[:, t].astype(jnp.float32)
    conv_in = jax.nn.silu(total)
    step_size = jax.nn.softplus(project(normed, step_proj) + step_bias)
    gate_in = project(normed, gate_proj).astype(jnp.bfloat16)
    head_count = step_size.shape[1]
    per_group = HEADS // GROUPS
    group_count = head_count // per_group
    flat = row_count * head_count

    def by_head(one):
        grouped = one.reshape(row_count, group_count, NSTATE)
        return jnp.repeat(grouped, per_group, axis=1).reshape(flat, NSTATE)

    write_map = by_head(maps[0])
    read_map = by_head(maps[1])
    write2 = jnp.concatenate([write_map, write_map], axis=1)
    read2 = jnp.concatenate([read_map, read_map], axis=1)
    values = conv_in.reshape(flat, HEAD)
    step_col = step_size.reshape(flat, 1)
    decay_col = jnp.exp(-decay_rate * step_size).reshape(flat, 1)
    skip_col = jnp.tile(skip_gain, row_count).reshape(flat, 1)
    state = head_state.reshape(flat, HEAD * NSTATE)
    owner = lax.broadcasted_iota(jnp.int32, (HEAD, HEAD * NSTATE), 1) // NSTATE
    spread = (owner == lax.broadcasted_iota(jnp.int32, owner.shape, 0)).astype(jnp.bfloat16)
    stepped = step_col * values
    overlap = jnp.sum(write_map * read_map, axis=1, keepdims=True)
    gated = decay_col * read_state(state, read2, spread) + stepped * overlap + skip_col * values
    gated = gated.reshape(row_count, head_count * HEAD) * jax.nn.silu(gate_in.astype(jnp.float32))
    wide = gated.shape[1] // group_count
    inner = jnp.concatenate(
        [rms_scale(gated[:, g * wide : (g + 1) * wide]) for g in range(group_count)], axis=1
    )
    inner_out = (inner * inner_gain).astype(jnp.bfloat16)
    partial_out = project(inner_out, mixer_out).astype(jnp.bfloat16)
    mixed = partial_out.astype(jnp.float32) + swap_cores(partial_out).astype(jnp.float32)
    hidden_mid = stream.astype(jnp.float32) + mixed
    ffn_in = (rms_scale(hidden_mid) * channel_gain).astype(jnp.bfloat16)
    half_width = feature_count // lax.axis_size("tp")
    own_half = lax.dynamic_slice_in_dim(ffn_in, core * half_width, half_width, 1)
    kept = lax.dynamic_slice_in_dim(hidden_mid, core * half_width, half_width, 1)
    own_half, stepped = lax.optimization_barrier((own_half, stepped))
    state_out = write_state(state, decay_col, stepped, write2, spread)

    expert = (lax.axis_index("ep") // (ep_size // EXPERTS)).astype(jnp.float32)
    all_rows = named.shape[0]
    matched = named[:, :TOP_K] == expert
    chosen = jnp.any(matched, axis=1)
    weight = jnp.sum(jnp.where(matched, named[:, TOP_K:], 0.0), axis=1)
    earlier = lax.broadcasted_iota(jnp.int32, (all_rows, all_rows), 0)
    later = lax.broadcasted_iota(jnp.int32, (all_rows, all_rows), 1)
    before = (earlier < later) & (earlier // row_count == later // row_count)
    rank = jnp.sum((before & chosen[:, None]).astype(jnp.int32), axis=0)
    slot = (jnp.arange(all_rows, dtype=jnp.int32) // row_count) * CAP + rank
    slots = lax.broadcasted_iota(jnp.int32, (ep_size * CAP, all_rows), 0)
    is_slot = (slots == slot[None, :]) & chosen[None, :]
    pick = is_slot.astype(jnp.bfloat16)
    slot_weight = jnp.sum(jnp.where(is_slot, weight[None, :], 0.0), axis=1)

    piece = gather_rows(own_half, dims)
    piece_other = swap_cores(piece)
    mine = project(pick, piece).astype(jnp.bfloat16)
    theirs = project(pick, piece_other).astype(jnp.bfloat16)
    first = core == 0
    taken = jnp.concatenate(
        [jnp.where(first, mine, theirs), jnp.where(first, theirs, mine)], axis=1
    )
    act = (
        jax.nn.silu(project(taken, expert_gate)) * project(taken, expert_up)
    ).astype(jnp.bfloat16)
    share = project(act, expert_down) * slot_weight[:, None]
    other_share = lax.dynamic_slice_in_dim(share, (1 - core) * half_width, half_width, 1)
    own_share = lax.dynamic_slice_in_dim(share, core * half_width, half_width, 1)
    came = swap_cores(other_share.astype(jnp.bfloat16))
    result = (own_share + came.astype(jnp.float32)).astype(jnp.bfloat16)

    gate_val = project(piece, dense_gate) + project(piece_other, gate_other)
    up_val = project(piece, dense_up) + project(piece_other, up_other)
    dense_act = (jax.nn.silu(gate_val) * up_val).astype(jnp.bfloat16)
    dense_res = project(dense_act, dense_down) * jax.nn.sigmoid(dense_mix)
    routed = lax.dot_general(
        pick, result, (((0,), (0,)), ((), ())), preferred_element_type=jnp.float32
    )
    updated = kept + scatter_rows(dense_res + routed, dims)
    return (updated.astype(jnp.bfloat16), state_out.reshape(head_state.shape))


def solution(mesh):
    placed = (
        P("ep", None),
        P(),
        P(None, "tp"),
        P(None, "tp"),
        P(None, None, "tp"),
        P(None, "tp"),
        P("tp"),
        P("tp"),
        P(None, "tp"),
        P(None, None, "tp"),
        P("ep", None, "tp"),
        P("ep", None, None, "tp"),
        P("ep", "tp", None),
        P("tp"),
        P("tp"),
        P("tp", None),
        P(),
        P("ep", None),
        P("ep", None),
        P(None, ("ep", "tp")),
        P(None, ("ep", "tp")),
        P(("ep", "tp"), None),
        P("tp", "ep"),
        P("tp", "ep"),
        P("ep", "tp"),
        P("tp"),
    )
    return jax.shard_map(
        local,
        mesh=mesh,
        in_specs=placed,
        out_specs=(P("ep", "tp"), P("ep", "tp", None)),
        check_vma=False,
    )
```
